32 devices in a mesh: ep: 8 (over z, core), tp: 4 (over y, x).
Axes of the slice: x: 2, y: 2, z: 4, core: 2. Of those that a mesh axis runs over, the one named last changes fastest.
Arguments:
- tokens: bfloat16 [128, 2048], P('ep'), may hold values from -6 to 6
- norm_gain: float32 [2048], replicated, may hold values from 0.1 to 1.9
- w_query: bfloat16 [2048, 512], P('ep', 'tp'), may hold values from -0.125 to 0.125
- w_key: bfloat16 [2048, 512], P('ep', 'tp'), may hold values from -0.125 to 0.125
- w_decay: bfloat16 [2048, 512], P('ep', 'tp'), may hold values from -0.125 to 0.125
- w_value: bfloat16 [2048, 1024], P('ep', 'tp'), may hold values from -0.125 to 0.125
- w_outgate: bfloat16 [2048, 1024], P('ep', 'tp'), may hold values from -0.125 to 0.125
- decay_rate: float32 [512], P('tp'), may hold values from 0.02 to 1
- state: float32 [128, 4, 128, 256], P('ep', 'tp'), may hold values from -15 to 15
- head_gain: float32 [256], replicated, may hold values from 0.1 to 1.9
- w_output: bfloat16 [1024, 2048], P('tp'), may hold values from -0.1875 to 0.1875
- moe_gain: float32 [2048], replicated, may hold values from 0.1 to 1.9
- expert_ids: int32 [128, 2], P('ep'), may hold values from 0 to 7, all different within a row; in each aligned block of 16 rows (0 to 15, 16 to 31, ...) at most 8 rows name the same one
- group_prob: float32 [128], P('ep'), may hold values from 0.3 to 1
- inner_prob: float32 [128, 2], P('ep'), may hold values from 0.05 to 1
- w_gate: bfloat16 [8, 2048, 2048], P('ep', None, 'tp'), may hold values from -0.125 to 0.125
- w_up: bfloat16 [8, 2048, 2048], P('ep', None, 'tp'), may hold values from -0.125 to 0.125
- w_down: bfloat16 [8, 2048, 2048], P('ep', 'tp'), may hold values from -0.125 to 0.125
Outputs:
- output: bfloat16 [128, 2048], P('ep', 'tp')
The draws below stay inside these ranges and needn't reach their ends.
Inputs may be any that keep to these rules, and one draw needn't show every extreme that they name: `expert_ids`: the 2 experts of a token differ. In the rows of one index of ep no expert is named more than 8 times, a bound that some block reaches there.
All inputs are finite; a program needn't handle non-finite values.
Results may differ from the reference program's by a relative error of at most 0.025.
Values may be sent and summed in bfloat16 or wider, within the bound.
A program may use at most 64 MiB of HBM per device.

```python
import math
import jax
import jax.numpy as jnp
import numpy as np
from jax import lax

D = 2048
DK = 128
DV = 256
GLA_HEADS = 4
FF = 2048
TOP = 2
SEQ_DEV = 16
SEQS = 128
EXPERTS = 8
CAP = 8
FF_BLOCK = 512
N_TP = 4


def shard_levels(key, shape, shards, low, top_value):
    def one(axis_at, shards_of):
        heights = jax.random.uniform(jax.random.fold_in(jax.random.fold_in(key, 6), axis_at), (shards_of,), jnp.float32, low / len(shards), top_value / len(shards))
        return jnp.repeat(jnp.exp(heights), shape[axis_at] // shards_of).reshape((-1,) + (1,) * (len(shape) - axis_at - 1))

    level = one(*shards[0])
    for cut in shards[1:]:
        level = level * one(*cut)
    return level


def routed_block(own_key, own, number, rows, amount, top, bound, lean):
    sequence = jax.random.permutation(own_key, amount)
    heavy_load, usual = shares(amount, rows * top, bound, lean, True), shares(amount, rows * top, bound, lean, False)
    places = jnp.arange(amount)

    def named(sizes, rotation):
        used = int((sizes > 0).sum())
        fixed = max(1, used // 4)
        passed = fixed + (places - fixed + rotation * (used - fixed)) % max(1, amount - fixed)
        return jnp.zeros((amount,), jnp.int32).at[sequence[jnp.where(places < fixed, places, passed)]].set(jnp.asarray(sizes, jnp.int32))

    sizes = jnp.where(number % 4 == 0, named(heavy_load, number // 4), named(usual, number - number // 4 - 1))
    mixed = jax.random.permutation(jax.random.fold_in(own, 3), amount)
    source_of, receiver = mixed[0:amount // 2 * 2:2], mixed[1:amount // 2 * 2:2]
    slack = jnp.minimum(sizes[source_of] - 1, bound - sizes[receiver]) // 2
    slack = jnp.where((source_of == sequence[0]) | (receiver == sequence[0]) | (sizes[receiver] == 0), 0, jnp.maximum(slack, 0))
    passed = jax.random.randint(jax.random.fold_in(own, 4), (amount // 2,), 0, 1 << 20) % (slack + 1)
    sizes = sizes.at[source_of].add(-passed).at[receiver].add(passed)
    items = jnp.searchsorted(jnp.cumsum(sizes), jnp.arange(rows * top), side="right").astype(jnp.int32)
    listing = items.reshape(top, rows).T
    listing = listing[jax.random.permutation(jax.random.fold_in(own, 1), rows)]
    rotation = jax.random.randint(jax.random.fold_in(own, 2), (rows, 1), 0, top)
    return jnp.take_along_axis(listing, (jnp.arange(top)[None, :] + rotation) % top, axis=1)


def shares(count, total, reach, skew, full):
    weights = [(1 << 20) // math.isqrt(standing ** skew) + 1 for standing in range(1, count + 1)]
    largest = reach if full else min(reach, max(-(-total // count), total * weights[0] // sum(weights)))
    least = 1 if total - largest >= count - 1 else 0
    holding, rest = [largest] + [least] * (count - 1), total - largest - least * (count - 1)
    while rest > 0:
        movable = [i for i in range(1, count) if holding[i] < largest] or [i for i in range(1, count) if holding[i] < reach]
        mass, budget = sum([weights[i] for i in movable]), rest
        for i in movable:
            addition = min(reach - holding[i], max(1, budget * weights[i] // mass), rest)
            holding[i] = holding[i] + addition
            rest = rest - addition
    return np.array(holding)


def scatter_about(rng, extent, width, limit, split=(), kind=jnp.bfloat16):
    result = width * jax.random.normal(rng, extent, jnp.float32)
    if split:
        result = result * shard_levels(rng, extent, split, -0.22, 0.18)
    return jnp.clip(result, -limit, limit).astype(kind)


def setup_inputs(seed: int = 0) -> dict:
    streams_of = jax.random.split(jax.random.key(seed), 19)
    tokens = scatter_about(streams_of[0], (SEQS, D), 1.0, 6.0, ((0, 8),))
    norm_gain = jnp.clip(1.0 + 0.18 * jax.random.normal(streams_of[1], (D,), jnp.float32), 0.1, 1.9)
    w_query = scatter_about(streams_of[2], (D, GLA_HEADS * DK), D ** -0.5, 0.125, ((0, 8), (1, 4)))
    w_key = scatter_about(streams_of[3], (D, GLA_HEADS * DK), D ** -0.5, 0.125, ((0, 8), (1, 4)))
    w_decay = scatter_about(streams_of[4], (D, GLA_HEADS * DK), D ** -0.5, 0.125, ((0, 8), (1, 4)))
    w_value = scatter_about(streams_of[5], (D, GLA_HEADS * DV), D ** -0.5, 0.125, ((0, 8), (1, 4)))
    w_outgate = scatter_about(streams_of[6], (D, GLA_HEADS * DV), D ** -0.5, 0.125, ((0, 8), (1, 4)))
    decay_rate = jnp.clip(jnp.exp(math.log(1.0) - 3.912023 * jax.random.uniform(streams_of[7], (GLA_HEADS * DK,), jnp.float32) ** shard_levels(streams_of[7], (GLA_HEADS * DK,), ((0, 4),), -0.2, 0.2)), 0.02, 1.0)
    state = scatter_about(streams_of[8], (SEQS, GLA_HEADS, DK, DV), 3.0, 15.0, ((0, 8), (1, 4)), jnp.float32)
    head_gain = jnp.clip(1.0 + 0.18 * jax.random.normal(streams_of[9], (DV,), jnp.float32), 0.1, 1.9)
    w_output = scatter_about(streams_of[10], (GLA_HEADS * DV, D), (GLA_HEADS * DV) ** -0.5, 0.1875, ((0, 4),))
    moe_gain = jnp.clip(1.0 + 0.18 * jax.random.normal(streams_of[11], (D,), jnp.float32), 0.1, 1.9)
    expert_ids_keys = jax.random.split(jax.random.fold_in(streams_of[12], 1), SEQS // SEQ_DEV)
    expert_ids_turns = jax.random.permutation(jax.random.fold_in(streams_of[12], 3), SEQS // SEQ_DEV)
    expert_ids = jax.vmap(lambda own, number: routed_block(jax.random.fold_in(streams_of[12], 2), own, number, SEQ_DEV, EXPERTS, TOP, CAP, 2))(expert_ids_keys, expert_ids_turns).reshape((SEQS, TOP))
    group_prob = jnp.clip(0.3 + 0.7 * jax.random.uniform(streams_of[13], (SEQS,), jnp.float32) ** shard_levels(streams_of[13], (SEQS,), ((0, 8),), -0.2, 0.2), 0.3, 1.0)
    inner_prob = jnp.clip(0.05 + 0.95 * jax.random.uniform(streams_of[14], (SEQS, TOP), jnp.float32) ** shard_levels(streams_of[14], (SEQS, TOP), ((0, 8),), -0.2, 0.2), 0.05, 1.0)
    w_gate = scatter_about(streams_of[15], (EXPERTS, D, FF), D ** -0.5, 0.125, ((0, 8), (2, 4)))
    w_up = scatter_about(streams_of[16], (EXPERTS, D, FF), D ** -0.5, 0.125, ((0, 8), (2, 4)))
    w_down = scatter_about(streams_of[17], (EXPERTS, FF, D), FF ** -0.5, 0.125, ((0, 8), (1, 4)))
    return {"tokens": tokens, "norm_gain": norm_gain, "w_query": w_query, "w_key": w_key, "w_decay": w_decay, "w_value": w_value, "w_outgate": w_outgate, "decay_rate": decay_rate, "state": state, "head_gain": head_gain, "w_output": w_output, "moe_gain": moe_gain, "expert_ids": expert_ids, "group_prob": group_prob, "inner_prob": inner_prob, "w_gate": w_gate, "w_up": w_up, "w_down": w_down}


epsilon = 1e-05

def inverse_rms(values):
    return lax.rsqrt(lax.optimization_barrier(jnp.mean(values * values, axis=-1, keepdims=True)) + epsilon)

def reference(tokens, norm_gain, w_query, w_key, w_decay, w_value, w_outgate, decay_rate, state, head_gain, w_output, moe_gain, expert_ids, group_prob, inner_prob, w_gate, w_up, w_down):
    wide = jnp.float32
    narrow = jnp.bfloat16
    residual = tokens.astype(wide)
    normed = (residual * inverse_rms(residual) * norm_gain.astype(wide)).astype(narrow)

    def project(weight):
        return jnp.dot(normed, weight, preferred_element_type=wide)
    query = project(w_query).astype(narrow).astype(wide).reshape(SEQS, GLA_HEADS, DK) * DK ** (-0.5)
    key_rows = project(w_key).astype(narrow).astype(wide).reshape(SEQS, GLA_HEADS, DK)
    value_rows = project(w_value).astype(narrow).astype(wide).reshape(SEQS, GLA_HEADS, DV)
    gate_rows = project(w_outgate).astype(narrow).astype(wide).reshape(SEQS, GLA_HEADS, DV)
    decay_log = jax.nn.log_sigmoid(project(w_decay)) * decay_rate
    decay = jnp.exp(decay_log).reshape(SEQS, GLA_HEADS, DK)
    updated = decay[..., None] * state + key_rows[..., None] * value_rows[:, :, None, :]
    readout = jnp.einsum('shk,shkv->shv', query, updated, precision=lax.Precision.HIGHEST)
    gated = (readout * inverse_rms(readout) * head_gain.astype(wide) * jax.nn.silu(gate_rows)).astype(narrow)
    per_head = jnp.einsum('shv,hvd->shd', gated.astype(wide), w_output.astype(wide).reshape(GLA_HEADS, DV, D))
    attention = lax.optimization_barrier(jnp.sum(per_head.astype(narrow).astype(wide), axis=1))
    mixed = (residual + attention).astype(narrow)
    mixed_wide = mixed.astype(wide)
    moe_in = (mixed_wide * inverse_rms(mixed_wide) * moe_gain.astype(wide)).astype(narrow)
    route_weight = group_prob[:, None] * inner_prob / lax.optimization_barrier(jnp.sum(inner_prob, axis=1, keepdims=True))
    slot_total = EXPERTS * CAP

    def one_expert(total, inputs):
        weight_gate, weight_up, weight_down, index = inputs
        chosen = expert_ids == index
        coeff = lax.optimization_barrier(jnp.sum(jnp.where(chosen, route_weight, 0.0), axis=1))
        marks = jnp.where(jnp.any(chosen, axis=1), 0, 1).astype(jnp.int32)
        order = jnp.argsort(marks, stable=True)[:slot_total].astype(jnp.int32)
        rows = moe_in[order]
        gate = jnp.dot(rows, weight_gate, preferred_element_type=wide)
        upper = jnp.dot(rows, weight_up, preferred_element_type=wide)
        hidden = (jax.nn.silu(gate) * upper).astype(narrow)
        pieces = jnp.einsum('rbf,bfd->rbd', hidden.astype(wide).reshape(slot_total, N_TP, FF_BLOCK), weight_down.astype(wide).reshape(N_TP, FF_BLOCK, D))
        expert_out = lax.optimization_barrier(jnp.sum(pieces.astype(narrow).astype(wide), axis=1)).astype(narrow).astype(wide)
        total = total.at[order].add(coeff[order][:, None] * expert_out)
        return (total, None)
    experts_sum, _ = lax.scan(one_expert, jnp.zeros((SEQS, D), wide), (w_gate, w_up, w_down, jnp.arange(EXPERTS, dtype=jnp.int32)))
    return (mixed_wide + experts_sum).astype(narrow)
```

```python
import functools

import jax
import jax.numpy as jnp
from jax import lax
from jax.experimental import pallas as pl
from jax.experimental.pallas import tpu as pltpu
from jax.sharding import PartitionSpec as P

epsilon = 1e-05
MESH = pl.DeviceIdType.MESH
WIDE = jnp.float32
NARROW = jnp.bfloat16


def inverse_rms(values):
    return lax.rsqrt(jnp.mean(values * values, axis=-1, keepdims=True) + epsilon)


def silu(values):
    return values / (1.0 + jnp.exp(-values))


def column(row):
    count = row.shape[1]
    shape = (count, count)
    diagonal = lax.broadcasted_iota(jnp.int32, shape, 0) == lax.broadcasted_iota(jnp.int32, shape, 1)
    return jnp.sum(jnp.where(diagonal, jnp.broadcast_to(row, shape), 0.0), axis=1, keepdims=True)


def layer(
    ep,
    tp,
    capacity,
    tokens_in, norm_gain_in, w_query_in, w_key_in, w_decay_in, w_value_in, w_outgate_in,
    decay_rate_in, state_in, head_gain_in, w_output_in, moe_gain_in, ids_in, group_in, inner_in,
    w_gate_in, w_up_in, w_down_in,
    out_ref,
    tokens, norm_gain, w_project, decay_rate, state, head_gain, w_output, moe_gain, ids, group,
    inner, w_gate, w_up, w_down,
    send1, recv1, send2, recv2, readout_rows, send3, recv3, mixed_rows, pack, send4, recv4, send6,
    recv6, pack_out, send7, recv7,
    local_sems, s1, r1, s2, r2, s3, r3, s4, r4, s6, r6, s7, r7,
):
    me_ep = lax.axis_index("ep")
    me_tp = lax.axis_index("tp")
    ahead_ep = [lax.rem(me_ep + o, ep) for o in range(ep)]
    behind_ep = [lax.rem(me_ep + ep - o, ep) for o in range(ep)]
    ahead_tp = [lax.rem(me_tp + o, tp) for o in range(tp)]

    query_cols = w_query_in.shape[1]
    value_cols = w_value_in.shape[1]
    edges = [0, query_cols, 2 * query_cols, 3 * query_cols, 3 * query_cols + value_cols,
             3 * query_cols + 2 * value_cols]
    loads = [
        (tokens_in, tokens),
        (norm_gain_in, norm_gain),
        (w_query_in, w_project.at[:, edges[0]:edges[1]]),
        (w_key_in, w_project.at[:, edges[1]:edges[2]]),
        (w_decay_in, w_project.at[:, edges[2]:edges[3]]),
        (w_value_in, w_project.at[:, edges[3]:edges[4]]),
        (w_outgate_in, w_project.at[:, edges[4]:edges[5]]),
        (decay_rate_in, decay_rate),
        (state_in, state),
        (head_gain_in, head_gain),
        (w_output_in, w_output),
        (moe_gain_in, moe_gain),
        (ids_in, ids),
        (group_in, group),
        (inner_in, inner),
        (w_gate_in.at[0], w_gate),
        (w_up_in.at[0], w_up),
        (w_down_in.at[0], w_down),
    ]
    loads = [
        pltpu.make_async_copy(source, target, local_sems.at[i])
        for i, (source, target) in enumerate(loads)
    ]
    for load in loads[:2]:
        load.start()

    barrier = pltpu.get_barrier_semaphore()
    for o in range(1, ep):
        pl.semaphore_signal(barrier, inc=1, device_id={"ep": ahead_ep[o]}, device_id_type=MESH)
    for o in range(1, tp):
        pl.semaphore_signal(barrier, inc=1, device_id={"tp": ahead_tp[o]}, device_id_type=MESH)

    for load in loads[2:]:
        load.start()

    def remote(source, target, send_sem, recv_sem, device):
        copy = pltpu.make_async_remote_copy(
            src_ref=source, dst_ref=target, send_sem=send_sem, recv_sem=recv_sem,
            device_id=device, device_id_type=MESH,
        )
        copy.start()
        return copy

    loads[0].wait()
    loads[1].wait()
    rows = tokens.shape[0]
    width = tokens.shape[1]
    slice_width = width // ep
    residual = tokens[...].astype(WIDE)
    normed = (residual * inverse_rms(residual) * norm_gain[...]).astype(NARROW)
    for e in range(ep):
        send1[e] = normed[:, e * slice_width:(e + 1) * slice_width]
    pl.semaphore_wait(barrier, ep - 1 + tp - 1)
    pending = []
    first = [
        remote(send1.at[ahead_ep[o]], recv1.at[o], s1.at[o], r1.at[o], {"ep": ahead_ep[o]})
        for o in range(1, ep)
    ]
    pending += first
    recv1[0] = send1[me_ep]

    for i in (12, 13, 14):
        loads[i].wait()
    slots = ep * capacity
    row_of = lax.broadcasted_iota(jnp.int32, (rows, slots), 1)
    expert_of = lax.rem(me_ep + row_of // capacity, ep)
    place_of = lax.rem(row_of, capacity).astype(WIDE)
    probs = inner[...]
    scale = column(group[...]) / jnp.sum(probs, axis=1, keepdims=True)
    names = ids[...]
    hits = jnp.zeros((rows, slots), WIDE)
    weights = jnp.zeros((rows, slots), WIDE)
    for k in range(names.shape[1]):
        chosen = names[:, k:k + 1] == expert_of
        hits = jnp.where(chosen, 1.0, hits)
        weights = jnp.where(chosen, scale * probs[:, k:k + 1], weights)
    square = (rows, rows)
    earlier = jnp.where(
        lax.broadcasted_iota(jnp.int32, square, 1) < lax.broadcasted_iota(jnp.int32, square, 0),
        1.0, 0.0,
    )
    rank = jnp.dot(earlier.astype(NARROW), hits.astype(NARROW), preferred_element_type=WIDE)
    held = jnp.where(jnp.abs(rank - place_of) < 0.5, hits, 0.0)
    combine = held * weights
    select = held.astype(NARROW)

    for i in range(2, 7):
        loads[i].wait()
    for copy in first:
        copy.wait_recv()
    spread = recv1[...].reshape(ep * rows, slice_width)
    partial = jnp.dot(spread, w_project[...], preferred_element_type=WIDE)
    send2[...] = partial.astype(NARROW).reshape(ep, rows, edges[5])
    second = [
        remote(send2.at[o], recv2.at[o], s2.at[o], r2.at[o], {"ep": behind_ep[o]})
        for o in range(1, ep)
    ]
    pending += second
    for i in (7, 8, 9, 10, 11):
        loads[i].wait()
    projected = partial[0:rows]
    for copy in second:
        copy.wait_recv()
    for o in range(1, ep):
        projected = projected + recv2[o].astype(WIDE)

    heads, key_width, value_width = state.shape[1], state.shape[2], state.shape[3]
    query = projected[:, edges[0]:edges[1]].astype(NARROW).astype(WIDE) * key_width ** (-0.5)
    key_rows = projected[:, edges[1]:edges[2]].astype(NARROW).astype(WIDE)
    decay_pre = projected[:, edges[2]:edges[3]]
    value_rows = projected[:, edges[3]:edges[4]].astype(NARROW).astype(WIDE)
    gate_rows = projected[:, edges[4]:edges[5]].astype(NARROW).astype(WIDE)
    decay_log = jnp.minimum(decay_pre, 0.0) - jnp.log(1.0 + jnp.exp(-jnp.abs(decay_pre)))
    decayed = query * jnp.exp(decay_log * decay_rate[...])
    gated = []
    for h in range(heads):
        keys = slice(h * key_width, (h + 1) * key_width)
        values = slice(h * value_width, (h + 1) * value_width)
        factors = decayed[:, keys].T
        for s in range(rows):
            readout_rows[s:s + 1, :] = jnp.sum(
                factors[:, s:s + 1] * state[s, h], axis=0, keepdims=True
            )
        overlap = jnp.sum(query[:, keys] * key_rows[:, keys], axis=1, keepdims=True)
        readout = readout_rows[...] + overlap * value_rows[:, values]
        gated.append(
            (readout * inverse_rms(readout) * head_gain[...] * silu(gate_rows[:, values])).astype(NARROW)
        )
    gated = gated[0] if heads == 1 else jnp.concatenate(gated, axis=1)

    send3[...] = jnp.dot(gated, w_output[...], preferred_element_type=WIDE).astype(NARROW)
    third = [
        remote(send3, recv3.at[o], s3.at[o], r3.at[o], {"tp": ahead_tp[o]}) for o in range(1, tp)
    ]
    pending += third
    attention = send3[...].astype(WIDE)
    for copy in third:
        copy.wait_recv()
    for o in range(1, tp):
        attention = attention + recv3[o].astype(WIDE)
    mixed = (residual + attention).astype(NARROW).astype(WIDE)
    mixed_rows[...] = mixed
    moe_in = (mixed * inverse_rms(mixed) * moe_gain[...]).astype(NARROW)

    pack[...] = lax.dot_general(
        select, moe_in, (((0,), (0,)), ((), ())), preferred_element_type=WIDE
    )
    fourth = []
    for o in range(1, ep):
        send4[o] = pack[o * capacity:(o + 1) * capacity, :].astype(NARROW)
    for o in range(1, ep):
        fourth.append(
            remote(send4.at[o], recv4.at[o], s4.at[o], r4.at[o], {"ep": ahead_ep[o]})
        )
    pending += fourth
    for i in (15, 16, 17):
        loads[i].wait()
    for copy in fourth:
        copy.wait_recv()
    for o in range(1, ep):
        pack[o * capacity:(o + 1) * capacity, :] = recv4[o].astype(WIDE)
    arrived = pack[...].astype(NARROW)

    gate = jnp.dot(arrived, w_gate[...], preferred_element_type=WIDE)
    upper = jnp.dot(arrived, w_up[...], preferred_element_type=WIDE)
    hidden = (silu(gate) * upper).astype(NARROW)
    col_width = width // tp

    def block(o):
        start = pl.multiple_of(ahead_tp[o] * col_width, 128)
        return jnp.dot(
            hidden, w_down[:, pl.ds(start, col_width)], preferred_element_type=WIDE
        ).astype(NARROW)

    sixth = []
    for o in range(1, tp):
        send6[o] = block(o)
        sixth.append(remote(send6.at[o], recv6.at[o], s6.at[o], r6.at[o], {"tp": ahead_tp[o]}))
    pending += sixth
    expert_out = block(0).astype(WIDE)
    for copy in sixth:
        copy.wait_recv()
    for o in range(1, tp):
        expert_out = expert_out + recv6[o].astype(WIDE)
    pack_out[...] = expert_out.astype(NARROW).astype(WIDE)

    seventh = []
    for o in range(1, ep):
        send7[o] = pack_out[o * capacity:(o + 1) * capacity, :].astype(NARROW)
    for o in range(1, ep):
        seventh.append(
            remote(send7.at[o], recv7.at[o], s7.at[o], r7.at[o], {"ep": behind_ep[o]})
        )
    pending += seventh
    own = mixed_rows[:, pl.ds(pl.multiple_of(me_tp * col_width, 128), col_width)]
    for copy in seventh:
        copy.wait_recv()
    for o in range(1, ep):
        pack_out[o * capacity:(o + 1) * capacity, :] = recv7[o].astype(WIDE)
    moe_sum = jnp.dot(
        combine, pack_out[...], precision=lax.Precision.HIGHEST, preferred_element_type=WIDE
    )
    out_ref[...] = (own + moe_sum).astype(NARROW)
    for copy in pending:
        copy.wait_send()


def on_device(
    tokens, norm_gain, w_query, w_key, w_decay, w_value, w_outgate, decay_rate, state, head_gain,
    w_output, moe_gain, expert_ids, group_prob, inner_prob, w_gate, w_up, w_down,
):
    ep = lax.axis_size("ep")
    tp = lax.axis_size("tp")
    rows, width = tokens.shape
    top = expert_ids.shape[1]
    capacity = 2 * rows * top // ep
    slots = ep * capacity
    col_width = width // tp
    project_cols = 3 * w_query.shape[1] + 2 * w_value.shape[1]
    hidden = w_gate.shape[2]
    operands = (
        tokens, norm_gain.reshape(1, -1), w_query, w_key, w_decay, w_value, w_outgate,
        decay_rate.reshape(1, -1), state, head_gain.reshape(1, -1), w_output,
        moe_gain.reshape(1, -1), expert_ids, group_prob.reshape(1, -1), inner_prob, w_gate, w_up,
        w_down,
    )
    vmem = pltpu.VMEM
    local = [
        vmem((rows, width), NARROW),
        vmem((1, width), WIDE),
        vmem((w_query.shape[0], project_cols), NARROW),
        vmem((1, decay_rate.shape[0]), WIDE),
        vmem(state.shape, WIDE),
        vmem((1, head_gain.shape[0]), WIDE),
        vmem(w_output.shape, NARROW),
        vmem((1, width), WIDE),
        vmem(expert_ids.shape, jnp.int32),
        vmem((1, rows), WIDE),
        vmem(inner_prob.shape, WIDE),
        vmem((width, hidden), NARROW),
        vmem((width, hidden), NARROW),
        vmem((hidden, width), NARROW),
    ]
    buffers = [
        vmem((ep, rows, width // ep), NARROW),
        vmem((ep, rows, width // ep), NARROW),
        vmem((ep, rows, project_cols), NARROW),
        vmem((ep, rows, project_cols), NARROW),
        vmem((rows, state.shape[3]), WIDE),
        vmem((rows, width), NARROW),
        vmem((tp, rows, width), NARROW),
        vmem((rows, width), WIDE),
        vmem((slots, width), WIDE),
        vmem((ep, capacity, width), NARROW),
        vmem((ep, capacity, width), NARROW),
        vmem((tp, slots, col_width), NARROW),
        vmem((tp, slots, col_width), NARROW),
        vmem((slots, col_width), WIDE),
        vmem((ep, capacity, col_width), NARROW),
        vmem((ep, capacity, col_width), NARROW),
    ]
    dma = pltpu.SemaphoreType.DMA
    along_ep, along_tp = [dma((ep,))] * 2, [dma((tp,))] * 2
    semaphores = (
        [dma((len(operands),))] + along_ep + along_ep + along_tp + along_ep + along_tp + along_ep
    )
    return pl.pallas_call(
        functools.partial(layer, ep, tp, capacity),
        out_shape=jax.ShapeDtypeStruct((rows, col_width), NARROW),
        in_specs=[pl.BlockSpec(memory_space=pl.ANY)] * len(operands),
        out_specs=pl.BlockSpec(memory_space=pltpu.VMEM),
        scratch_shapes=local + buffers + semaphores,
        compiler_params=pltpu.CompilerParams(
            collective_id=0, has_side_effects=True, vmem_limit_bytes=60 * 1024 * 1024
        ),
    )(*operands)


def solution(mesh):
    placed = (
        P("ep", None),
        P(),
        P("ep", "tp"),
        P("ep", "tp"),
        P("ep", "tp"),
        P("ep", "tp"),
        P("ep", "tp"),
        P("tp"),
        P("ep", "tp", None, None),
        P(),
        P("tp", None),
        P(),
        P("ep", None),
        P("ep"),
        P("ep", None),
        P("ep", None, "tp"),
        P("ep", None, "tp"),
        P("ep", "tp", None),
    )
    return jax.shard_map(
        on_device, mesh=mesh, in_specs=placed, out_specs=P("ep", "tp"), check_vma=False
    )
```

```python
import functools

import jax
import jax.numpy as jnp
from jax import lax
from jax.experimental import pallas as pl
from jax.experimental.pallas import tpu as pltpu
from jax.sharding import PartitionSpec as P

epsilon = 1e-05
MESH = pl.DeviceIdType.MESH
WIDE = jnp.float32
NARROW = jnp.bfloat16


def inverse_rms(values):
    return lax.rsqrt(jnp.mean(values * values, axis=-1, keepdims=True) + epsilon)


def silu(values):
    return values / (1.0 + jnp.exp(-values))


def column(row):
    count = row.shape[1]
    shape = (count, count)
    diagonal = lax.broadcasted_iota(jnp.int32, shape, 0) == lax.broadcasted_iota(jnp.int32, shape, 1)
    return jnp.sum(jnp.where(diagonal, jnp.broadcast_to(row, shape), jnp.zeros(shape, row.dtype)), axis=1, keepdims=True)


def flipped(index, bits):
    result, weight = index, 1
    while weight <= bits:
        if bits & weight:
            result = result + weight * (1 - 2 * lax.rem(index // weight, 2))
        weight *= 2
    return result


def layer(
    ep,
    tp,
    capacity,
    tokens_in, norm_gain_in, w_query_in, w_key_in, w_decay_in, w_value_in, w_outgate_in,
    decay_rate_in, state_in, head_gain_in, w_output_in, moe_gain_in, ids_in, group_in, inner_in,
    w_gate_in, w_up_in, w_down_in,
    out_ref,
    tokens, norm_gain, w_project, decay_rate, state, head_gain, w_output, moe_gain, ids, group,
    inner, w_gate, w_up, w_down,
    send1, recv1, send_pair, recv_pair, send2, recv2, readout_rows, send3, recv3, pack, send4, recv4, recv5, send_sum,
    recv_sum, send_scale, recv_scale, send6, recv6, pack_out, send7, recv7,
    local_sems, s1, r1, s2, r2, s3, r3, s4, r4, s5, r5, s_sum, r_sum, s_scale, r_scale, s6, r6, s7,
    r7,
):
    me_ep = lax.axis_index("ep")
    me_tp = lax.axis_index("tp")
    ahead_ep = behind_ep = [flipped(me_ep, o) for o in range(ep)]
    ahead_tp = [flipped(me_tp, o) for o in range(tp)]
    far_tp = list(reversed(range(1, tp)))

    query_cols = w_query_in.shape[1]
    value_cols = w_value_in.shape[1]
    edges = [0, query_cols, 2 * query_cols, 3 * query_cols, 3 * query_cols + value_cols,
             3 * query_cols + 2 * value_cols]
    loads = [
        (tokens_in, tokens),
        (norm_gain_in, norm_gain),
        (w_query_in, w_project.at[:, edges[0]:edges[1]]),
        (w_key_in, w_project.at[:, edges[1]:edges[2]]),
        (w_decay_in, w_project.at[:, edges[2]:edges[3]]),
        (w_value_in, w_project.at[:, edges[3]:edges[4]]),
        (w_outgate_in, w_project.at[:, edges[4]:edges[5]]),
        (decay_rate_in, decay_rate),
        (state_in, state),
        (head_gain_in, head_gain),
        (w_output_in, w_output),
        (moe_gain_in, moe_gain),
        (ids_in, ids),
        (group_in, group),
        (inner_in, inner),
        (w_gate_in.at[0], w_gate),
        (w_up_in.at[0], w_up),
        (w_down_in.at[0], w_down),
    ]
    loads = [
        pltpu.make_async_copy(source, target, local_sems.at[i])
        for i, (source, target) in enumerate(loads)
    ]
    for load in loads[:2]:
        load.start()

    barrier = pltpu.get_barrier_semaphore()
    for o in range(1, ep):
        pl.semaphore_signal(barrier, inc=1, device_id={"ep": ahead_ep[o]}, device_id_type=MESH)
    for o in range(1, tp):
        pl.semaphore_signal(barrier, inc=1, device_id={"tp": ahead_tp[o]}, device_id_type=MESH)

    for load in loads[2:]:
        load.start()

    def remote(source, target, send_sem, recv_sem, device):
        copy = pltpu.make_async_remote_copy(
            src_ref=source, dst_ref=target, send_sem=send_sem, recv_sem=recv_sem,
            device_id=device, device_id_type=MESH,
        )
        copy.start()
        return copy

    loads[0].wait()
    loads[1].wait()
    rows = tokens.shape[0]
    half = ep // 2
    width = tokens.shape[1]
    slice_width = width // ep
    residual = tokens[...].astype(WIDE)
    normed = (residual * inverse_rms(residual) * norm_gain[...]).astype(NARROW)
    for e in range(ep):
        send1[e] = normed[:, e * slice_width:(e + 1) * slice_width]
    pl.semaphore_wait(barrier, ep - 1 + tp - 1)
    pending = []
    first = [
        remote(send1.at[ahead_ep[o]], recv1.at[o // 2 + o % 2 * half], s1.at[o], r1.at[o], {"ep": ahead_ep[o]})
        for o in reversed(range(1, ep))
    ]
    pending += first
    recv1[0] = send1[me_ep]

    for i in (12, 13, 14):
        loads[i].wait()
    slots = ep * capacity
    groups = min(ep, 8)
    group_size = ep // groups
    row_of = lax.broadcasted_iota(jnp.int32, (rows, slots), 1)
    expert_of = jnp.zeros((rows, slots), jnp.int32)
    for o in range(ep):
        expert_of = jnp.where(row_of // capacity == o, ahead_ep[o], expert_of)
    place_of = lax.rem(row_of, capacity).astype(WIDE)
    top = ids.shape[0]
    probs = [column(inner[k:k + 1, :]) for k in range(top)]
    scale = column(group[...]) / functools.reduce(jnp.add, probs)
    names = [column(ids[k:k + 1, :]) for k in range(top)]
    hits = jnp.zeros((rows, slots), WIDE)
    weights = jnp.zeros((rows, slots), WIDE)
    for k in range(top):
        chosen = names[k] == expert_of
        hits = jnp.where(chosen, 1.0, hits)
        weights = jnp.where(chosen, scale * probs[k], weights)
    square = (rows, rows)
    diagonal = lax.broadcasted_iota(jnp.int32, square, 1) == lax.broadcasted_iota(jnp.int32, square, 0)
    earlier = jnp.where(
        lax.broadcasted_iota(jnp.int32, square, 1) < lax.broadcasted_iota(jnp.int32, square, 0),
        1.0, 0.0,
    )
    rank = jnp.dot(earlier.astype(NARROW), hits.astype(NARROW), preferred_element_type=WIDE)
    held = jnp.where(jnp.abs(rank - place_of) < 0.5, hits, 0.0)
    combine = held * weights
    select = held.astype(NARROW)

    for i in range(2, 7):
        loads[i].wait()
    for copy in first:
        copy.wait_recv()
    spread = recv1[...].reshape(ep * rows, slice_width)
    partial = jnp.dot(spread[half * rows:], w_project[...], preferred_element_type=WIDE)
    send_pair[...] = partial.astype(NARROW).reshape(half, rows, edges[5])
    pair = remote(send_pair, recv_pair, s2.at[0], r2.at[0], {"ep": ahead_ep[1]})
    pending.append(pair)
    partial = jnp.dot(spread[:half * rows], w_project[...], preferred_element_type=WIDE)
    pair.wait_recv()
    second = []
    for j in reversed(range(1, half)):
        send2[j] = (partial[j * rows:(j + 1) * rows] + recv_pair[j].astype(WIDE)).astype(NARROW)
        second.append(
            remote(send2.at[j], recv2.at[j], s2.at[j], r2.at[j], {"ep": ahead_ep[2 * j]})
        )
    pending += second
    projected = partial[:rows] + recv_pair[0].astype(WIDE)
    for i in (7, 8, 9, 10, 11):
        loads[i].wait()
    for copy in second:
        copy.wait_recv()
    for j in range(1, half):
        projected = projected + recv2[j].astype(WIDE)

    heads, key_width, value_width = state.shape[1], state.shape[2], state.shape[3]
    query = projected[:, edges[0]:edges[1]].astype(NARROW).astype(WIDE) * key_width ** (-0.5)
    key_rows = projected[:, edges[1]:edges[2]].astype(NARROW).astype(WIDE)
    decay_pre = projected[:, edges[2]:edges[3]]
    value_rows = projected[:, edges[3]:edges[4]].astype(NARROW).astype(WIDE)
    gate_rows = projected[:, edges[4]:edges[5]].astype(NARROW).astype(WIDE)
    decay_log = jnp.minimum(decay_pre, 0.0) - jnp.log(1.0 + jnp.exp(-jnp.abs(decay_pre)))
    decayed = query * jnp.exp(decay_log * decay_rate[...])
    gated = []
    for h in range(heads):
        keys = slice(h * key_width, (h + 1) * key_width)
        values = slice(h * value_width, (h + 1) * value_width)
        factors = decayed[:, keys].T
        for s in range(rows):
            readout_rows[s:s + 1, :] = jnp.sum(
                factors[:, s:s + 1] * state[s, h], axis=0, keepdims=True
            )
        overlap = jnp.sum(query[:, keys] * key_rows[:, keys], axis=1, keepdims=True)
        readout = readout_rows[...] + overlap * value_rows[:, values]
        gated.append(
            (readout * inverse_rms(readout) * head_gain[...] * silu(gate_rows[:, values])).astype(NARROW)
        )
    gated = gated[0] if heads == 1 else jnp.concatenate(gated, axis=1)

    col_width = width // tp

    def columns(o):
        return pl.ds(pl.multiple_of(ahead_tp[o] * col_width, 128), col_width)

    parts = jnp.dot(gated, w_output[...], preferred_element_type=WIDE).astype(NARROW)
    for p in range(tp):
        send3[p] = parts[:, p * col_width:(p + 1) * col_width]
    third = [
        remote(send3.at[ahead_tp[o]], recv3.at[o], s3.at[o], r3.at[o], {"tp": ahead_tp[o]})
        for o in far_tp
    ]
    pending += third
    attention = send3[me_tp].astype(WIDE)
    for copy in third:
        copy.wait_recv()
    for o in range(1, tp):
        attention = attention + recv3[o].astype(WIDE)
    mixed = (tokens[:, columns(0)].astype(WIDE) + attention).astype(NARROW).astype(WIDE)

    gained = (mixed * moe_gain[:, columns(0)]).astype(NARROW)
    pack[...] = lax.dot_general(
        select, gained, (((0,), (0,)), ((), ())), preferred_element_type=WIDE
    )
    for o in range(ep):
        target = send4 if o else recv4
        target[o] = pack[o * capacity:(o + 1) * capacity, :].astype(NARROW)
    fourth = [
        remote(send4.at[o], recv4.at[o], s4.at[o], r4.at[o], {"ep": ahead_ep[o]})
        for o in reversed(range(1, ep))
    ]
    pending += fourth

    squares = jnp.sum(mixed * mixed, axis=1, keepdims=True)
    send_sum[...] = jnp.sum(jnp.where(diagonal, squares, 0.0), axis=0, keepdims=True)
    sums = [
        remote(send_sum, recv_sum.at[o], s_sum.at[o], r_sum.at[o], {"tp": ahead_tp[o]})
        for o in range(1, tp)
    ]
    pending += sums

    fifth = []

    def forward(g):
        for o in far_tp:
            fifth.append(
                remote(
                    recv4.at[pl.ds(g * group_size, group_size)],
                    recv5.at[o, pl.ds(g * group_size, group_size)],
                    s5.at[o, g], r5.at[o, g], {"tp": ahead_tp[o]},
                )
            )

    if group_size == 1:
        forward(0)
    for copy in sums:
        copy.wait_recv()
    total = send_sum[...]
    for o in range(1, tp):
        total = total + recv_sum[o]
    scales = column(lax.rsqrt(total / width + epsilon))
    send_scale[...] = jnp.sum(held * scales, axis=0, keepdims=True)
    scaled = [
        remote(send_scale, recv_scale.at[o], s_scale.at[o], r_scale.at[o], {"ep": ahead_ep[o]})
        for o in reversed(range(1, ep))
    ]
    pending += scaled
    for g in range(1 if group_size == 1 else 0, groups):
        for o in range(max(1, g * group_size), (g + 1) * group_size):
            fourth[ep - 1 - o].wait_recv()
        forward(g)
    pending += fifth
    for i in (15, 16, 17):
        loads[i].wait()

    gate = jnp.zeros((slots, w_gate.shape[1]), WIDE)
    upper = gate
    for o in range(tp):
        if o:
            for g in range(groups):
                fifth[g * (tp - 1) + tp - 1 - o].wait_recv()
        for e in range(ep):
            pack[e * capacity:(e + 1) * capacity, :] = (recv5[o, e] if o else recv4[e]).astype(WIDE)
        arrived = pack[...].astype(NARROW)
        depth = pl.ds(
            pl.multiple_of(ahead_tp[o] * col_width, 128), col_width
        )
        gate = gate + jnp.dot(arrived, w_gate[depth, :], preferred_element_type=WIDE)
        upper = upper + jnp.dot(arrived, w_up[depth, :], preferred_element_type=WIDE)
    for copy in scaled:
        copy.wait_recv()
    slot_of = lax.broadcasted_iota(jnp.int32, (1, slots), 1) // capacity
    slot_scale = jnp.where(slot_of == 0, send_scale[...], 0.0)
    for o in range(1, ep):
        slot_scale = jnp.where(slot_of == o, recv_scale[o], slot_scale)
    slot_scale = column(slot_scale)
    gate = gate * slot_scale
    upper = upper * slot_scale
    hidden = (silu(gate) * upper).astype(NARROW)

    def block(o):
        return jnp.dot(
            hidden, w_down[:, columns(o)], preferred_element_type=WIDE
        ).astype(NARROW)

    sixth = []
    for o in far_tp:
        send6[o] = block(o)
        sixth.append(remote(send6.at[o], recv6.at[o], s6.at[o], r6.at[o], {"tp": ahead_tp[o]}))
    pending += sixth
    expert_out = block(0).astype(WIDE)
    for copy in sixth:
        copy.wait_recv()
    for o in range(1, tp):
        expert_out = expert_out + recv6[o].astype(WIDE)
    pack_out[...] = expert_out.astype(NARROW).astype(WIDE)

    seventh = []
    for o in range(1, ep):
        send7[o] = pack_out[o * capacity:(o + 1) * capacity, :].astype(NARROW)
    for o in reversed(range(1, ep)):
        seventh.append(
            remote(send7.at[o], recv7.at[o], s7.at[o], r7.at[o], {"ep": behind_ep[o]})
        )
    pending += seventh
    for copy in seventh:
        copy.wait_recv()
    for o in range(1, ep):
        pack_out[o * capacity:(o + 1) * capacity, :] = recv7[o].astype(WIDE)
    moe_sum = jnp.dot(
        combine, pack_out[...], precision=lax.Precision.HIGHEST, preferred_element_type=WIDE
    )
    out_ref[...] = (mixed + moe_sum).astype(NARROW)
    for copy in pending:
        copy.wait_send()


def on_device(
    tokens, norm_gain, w_query, w_key, w_decay, w_value, w_outgate, decay_rate, state, head_gain,
    w_output, moe_gain, expert_ids, group_prob, inner_prob, w_gate, w_up, w_down,
):
    ep = lax.axis_size("ep")
    tp = lax.axis_size("tp")
    rows, width = tokens.shape
    top = expert_ids.shape[1]
    capacity = 2 * rows * top // ep
    slots = ep * capacity
    col_width = width // tp
    project_cols = 3 * w_query.shape[1] + 2 * w_value.shape[1]
    hidden = w_gate.shape[2]
    operands = (
        tokens, norm_gain.reshape(1, -1), w_query, w_key, w_decay, w_value, w_outgate,
        decay_rate.reshape(1, -1), state, head_gain.reshape(1, -1), w_output,
        moe_gain.reshape(1, -1), expert_ids.T, group_prob.reshape(1, -1), inner_prob.T, w_gate, w_up,
        w_down,
    )
    vmem = pltpu.VMEM
    local = [
        vmem((rows, width), NARROW),
        vmem((1, width), WIDE),
        vmem((w_query.shape[0], project_cols), NARROW),
        vmem((1, decay_rate.shape[0]), WIDE),
        vmem(state.shape, WIDE),
        vmem((1, head_gain.shape[0]), WIDE),
        vmem(w_output.shape, NARROW),
        vmem((1, width), WIDE),
        vmem((top, rows), jnp.int32),
        vmem((1, rows), WIDE),
        vmem((top, rows), WIDE),
        vmem((width, hidden), NARROW),
        vmem((width, hidden), NARROW),
        vmem((hidden, width), NARROW),
    ]
    buffers = [
        vmem((ep, rows, width // ep), NARROW),
        vmem((ep, rows, width // ep), NARROW),
        vmem((ep // 2, rows, project_cols), NARROW),
        vmem((ep // 2, rows, project_cols), NARROW),
        vmem((ep // 2, rows, project_cols), NARROW),
        vmem((ep // 2, rows, project_cols), NARROW),
        vmem((rows, state.shape[3]), WIDE),
        vmem((tp, rows, col_width), NARROW),
        vmem((tp, rows, col_width), NARROW),
        vmem((slots, col_width), WIDE),
        vmem((ep, capacity, col_width), NARROW),
        vmem((ep, capacity, col_width), NARROW),
        vmem((tp, ep, capacity, col_width), NARROW),
        vmem((1, rows), WIDE),
        vmem((tp, 1, rows), WIDE),
        vmem((1, slots), WIDE),
        vmem((ep, 1, slots), WIDE),
        vmem((tp, slots, col_width), NARROW),
        vmem((tp, slots, col_width), NARROW),
        vmem((slots, col_width), WIDE),
        vmem((ep, capacity, col_width), NARROW),
        vmem((ep, capacity, col_width), NARROW),
    ]
    dma = pltpu.SemaphoreType.DMA
    along_ep, along_tp = [dma((ep,))] * 2, [dma((tp,))] * 2
    semaphores = (
        [dma((len(operands),))] + along_ep + along_ep + along_tp + along_ep
        + [dma((tp, min(ep, 8)))] * 2 + along_tp + along_ep + along_tp + along_ep
    )
    return pl.pallas_call(
        functools.partial(layer, ep, tp, capacity),
        out_shape=jax.ShapeDtypeStruct((rows, col_width), NARROW),
        in_specs=[pl.BlockSpec(memory_space=pl.ANY)] * len(operands),
        out_specs=pl.BlockSpec(memory_space=pltpu.VMEM),
        scratch_shapes=local + buffers + semaphores,
        compiler_params=pltpu.CompilerParams(
            collective_id=0, has_side_effects=True, vmem_limit_bytes=60 * 1024 * 1024
        ),
    )(*operands)


def solution(mesh):
    placed = (
        P("ep", None),
        P(),
        P("ep", "tp"),
        P("ep", "tp"),
        P("ep", "tp"),
        P("ep", "tp"),
        P("ep", "tp"),
        P("tp"),
        P("ep", "tp", None, None),
        P(),
        P("tp", None),
        P(),
        P("ep", None),
        P("ep"),
        P("ep", None),
        P("ep", None, "tp"),
        P("ep", None, "tp"),
        P("ep", "tp", None),
    )
    return jax.shard_map(
        on_device, mesh=mesh, in_specs=placed, out_specs=P("ep", "tp"), check_vma=False
    )
```

```python
import functools

import jax
import jax.numpy as jnp
from jax import lax
from jax.experimental import pallas as pl
from jax.experimental.pallas import tpu as pltpu
from jax.sharding import PartitionSpec as P

epsilon = 1e-05
MESH = pl.DeviceIdType.MESH
WIDE = jnp.float32
NARROW = jnp.bfloat16


def inverse_rms(values):
    return lax.rsqrt(jnp.mean(values * values, axis=-1, keepdims=True) + epsilon)


def silu(values):
    return values / (1.0 + jnp.exp(-values))


def column(row):
    count = row.shape[1]
    shape = (count, count)
    diagonal = lax.broadcasted_iota(jnp.int32, shape, 0) == lax.broadcasted_iota(jnp.int32, shape, 1)
    return jnp.sum(jnp.where(diagonal, jnp.broadcast_to(row, shape), jnp.zeros(shape, row.dtype)), axis=1, keepdims=True)


def flipped(index, bits):
    result, weight = index, 1
    while weight <= bits:
        if bits & weight:
            result = result + weight * (1 - 2 * lax.rem(index // weight, 2))
        weight *= 2
    return result


def layer(
    ep,
    tp,
    capacity,
    tokens_in, norm_gain_in, w_query_in, w_key_in, w_decay_in, w_value_in, w_outgate_in,
    decay_rate_in, state_in, head_gain_in, w_output_in, moe_gain_in, ids_in, group_in, inner_in,
    w_gate_in, w_up_in, w_down_in,
    out_ref,
    tokens, norm_gain, w_project, decay_rate, state, head_gain, w_output, moe_gain, ids, group,
    inner, w_gate, w_up, w_down,
    send1, recv1, send_pair, recv_pair, send2, recv2, readout_rows, send3, recv3, pack, send4, recv4, recv5, send_sum,
    recv_sum, send_scale, recv_scale, send6, recv6, pack_out, send7, recv7,
    local_sems, s1, r1, s2, r2, s3, r3, s4, r4, s5, r5, s_sum, r_sum, s_scale, r_scale, s6, r6, s7,
    r7,
):
    me_ep = lax.axis_index("ep")
    me_tp = lax.axis_index("tp")
    ahead_ep = behind_ep = [flipped(me_ep, o) for o in range(ep)]
    ahead_tp = [flipped(me_tp, o) for o in range(tp)]
    far_tp = list(reversed(range(1, tp)))

    query_cols = w_query_in.shape[1]
    value_cols = w_value_in.shape[1]
    edges = [0, query_cols, 2 * query_cols, 3 * query_cols, 3 * query_cols + value_cols,
             3 * query_cols + 2 * value_cols]
    loads = [
        (tokens_in, tokens),
        (norm_gain_in, norm_gain),
        (w_query_in, w_project.at[:, edges[0]:edges[1]]),
        (w_key_in, w_project.at[:, edges[1]:edges[2]]),
        (w_decay_in, w_project.at[:, edges[2]:edges[3]]),
        (w_value_in, w_project.at[:, edges[3]:edges[4]]),
        (w_outgate_in, w_project.at[:, edges[4]:edges[5]]),
        (decay_rate_in, decay_rate),
        (state_in, state),
        (head_gain_in, head_gain),
        (w_output_in, w_output),
        (moe_gain_in, moe_gain),
        (ids_in, ids),
        (group_in, group),
        (inner_in, inner),
        (w_gate_in.at[0], w_gate),
        (w_up_in.at[0], w_up),
        (w_down_in.at[0], w_down),
    ]
    loads = [
        pltpu.make_async_copy(source, target, local_sems.at[i])
        for i, (source, target) in enumerate(loads)
    ]
    for load in loads[:2]:
        load.start()

    barrier = pltpu.get_barrier_semaphore()
    for o in range(1, ep):
        pl.semaphore_signal(barrier, inc=1, device_id={"ep": ahead_ep[o]}, device_id_type=MESH)
    for o in range(1, tp):
        pl.semaphore_signal(barrier, inc=1, device_id={"tp": ahead_tp[o]}, device_id_type=MESH)

    for load in loads[2:]:
        load.start()

    def remote(source, target, send_sem, recv_sem, device):
        copy = pltpu.make_async_remote_copy(
            src_ref=source, dst_ref=target, send_sem=send_sem, recv_sem=recv_sem,
            device_id=device, device_id_type=MESH,
        )
        copy.start()
        return copy

    loads[0].wait()
    loads[1].wait()
    rows = tokens.shape[0]
    half = ep // 2
    width = tokens.shape[1]
    slice_width = width // ep
    residual = tokens[...].astype(WIDE)
    normed = (residual * inverse_rms(residual) * norm_gain[...]).astype(NARROW)
    for e in range(ep):
        send1[e] = normed[:, e * slice_width:(e + 1) * slice_width]
    pl.semaphore_wait(barrier, ep - 1 + tp - 1)
    pending = []
    first = [
        remote(send1.at[ahead_ep[o]], recv1.at[o // 2 + o % 2 * half], s1.at[o], r1.at[o], {"ep": ahead_ep[o]})
        for o in reversed(range(1, ep))
    ]
    pending += first
    recv1[0] = send1[me_ep]

    for i in (12, 13, 14):
        loads[i].wait()
    slots = ep * capacity
    groups = min(ep, 8)
    group_size = ep // groups
    row_of = lax.broadcasted_iota(jnp.int32, (rows, slots), 1)
    expert_of = jnp.zeros((rows, slots), jnp.int32)
    for o in range(ep):
        expert_of = jnp.where(row_of // capacity == o, ahead_ep[o], expert_of)
    place_of = lax.rem(row_of, capacity).astype(WIDE)
    top = ids.shape[0]
    probs = [column(inner[k:k + 1, :]) for k in range(top)]
    scale = column(group[...]) / functools.reduce(jnp.add, probs)
    names = [column(ids[k:k + 1, :]) for k in range(top)]
    hits = jnp.zeros((rows, slots), WIDE)
    weights = jnp.zeros((rows, slots), WIDE)
    for k in range(top):
        chosen = names[k] == expert_of
        hits = jnp.where(chosen, 1.0, hits)
        weights = jnp.where(chosen, scale * probs[k], weights)
    square = (rows, rows)
    diagonal = lax.broadcasted_iota(jnp.int32, square, 1) == lax.broadcasted_iota(jnp.int32, square, 0)
    earlier = jnp.where(
        lax.broadcasted_iota(jnp.int32, square, 1) < lax.broadcasted_iota(jnp.int32, square, 0),
        1.0, 0.0,
    )
    rank = jnp.dot(earlier.astype(NARROW), hits.astype(NARROW), preferred_element_type=WIDE)
    held = jnp.where(jnp.abs(rank - place_of) < 0.5, hits, 0.0)
    combine = held * weights
    select = held.astype(NARROW)

    for i in range(2, 7):
        loads[i].wait()
    for copy in first:
        copy.wait_recv()
    spread = recv1[...].reshape(ep * rows, slice_width)
    partial = jnp.dot(spread[half * rows:], w_project[...], preferred_element_type=WIDE)
    send_pair[...] = partial.astype(NARROW).reshape(half, rows, edges[5])
    pair = remote(send_pair, recv_pair, s2.at[0], r2.at[0], {"ep": ahead_ep[1]})
    pending.append(pair)
    partial = jnp.dot(spread[:half * rows], w_project[...], preferred_element_type=WIDE)
    pair.wait_recv()
    second = []
    for j in reversed(range(1, half)):
        send2[j] = (partial[j * rows:(j + 1) * rows] + recv_pair[j].astype(WIDE)).astype(NARROW)
        second.append(
            remote(send2.at[j], recv2.at[j], s2.at[j], r2.at[j], {"ep": ahead_ep[2 * j]})
        )
    pending += second
    projected = partial[:rows] + recv_pair[0].astype(WIDE)
    for i in (7, 8, 9, 10, 11):
        loads[i].wait()
    for copy in second:
        copy.wait_recv()
    for j in range(1, half):
        projected = projected + recv2[j].astype(WIDE)

    heads, key_width, value_width = state.shape[1], state.shape[2], state.shape[3]
    query = projected[:, edges[0]:edges[1]].astype(NARROW).astype(WIDE) * key_width ** (-0.5)
    key_rows = projected[:, edges[1]:edges[2]].astype(NARROW).astype(WIDE)
    decay_pre = projected[:, edges[2]:edges[3]]
    value_rows = projected[:, edges[3]:edges[4]].astype(NARROW).astype(WIDE)
    gate_rows = projected[:, edges[4]:edges[5]].astype(NARROW).astype(WIDE)
    decay_log = jnp.minimum(decay_pre, 0.0) - jnp.log(1.0 + jnp.exp(-jnp.abs(decay_pre)))
    decayed = query * jnp.exp(decay_log * decay_rate[...])
    gated = []
    for h in range(heads):
        keys = slice(h * key_width, (h + 1) * key_width)
        values = slice(h * value_width, (h + 1) * value_width)
        factors = decayed[:, keys].T
        for s in range(rows):
            readout_rows[s:s + 1, :] = jnp.sum(
                factors[:, s:s + 1] * state[s, h], axis=0, keepdims=True
            )
        overlap = jnp.sum(query[:, keys] * key_rows[:, keys], axis=1, keepdims=True)
        readout = readout_rows[...] + overlap * value_rows[:, values]
        gated.append(
            (readout * inverse_rms(readout) * head_gain[...] * silu(gate_rows[:, values])).astype(NARROW)
        )
    gated = gated[0] if heads == 1 else jnp.concatenate(gated, axis=1)

    col_width = width // tp

    def columns(o):
        return pl.ds(pl.multiple_of(ahead_tp[o] * col_width, 128), col_width)

    parts = jnp.dot(gated, w_output[...], preferred_element_type=WIDE).astype(NARROW)
    for p in range(tp):
        send3[p] = parts[:, p * col_width:(p + 1) * col_width]
    third = [
        remote(send3.at[ahead_tp[o]], recv3.at[o], s3.at[o], r3.at[o], {"tp": ahead_tp[o]})
        for o in far_tp
    ]
    pending += third
    attention = send3[me_tp].astype(WIDE)
    for copy in third:
        copy.wait_recv()
    for o in range(1, tp):
        attention = attention + recv3[o].astype(WIDE)
    mixed = (tokens[:, columns(0)].astype(WIDE) + attention).astype(NARROW).astype(WIDE)

    gained = (mixed * moe_gain[:, columns(0)]).astype(NARROW)
    pack[...] = lax.dot_general(
        select, gained, (((0,), (0,)), ((), ())), preferred_element_type=WIDE
    )
    for o in range(ep):
        target = send4 if o else recv4
        target[o] = pack[o * capacity:(o + 1) * capacity, :].astype(NARROW)
    fourth = [
        remote(send4.at[o], recv4.at[o], s4.at[o], r4.at[o], {"ep": ahead_ep[o]})
        for o in reversed(range(1, ep))
    ]
    pending += fourth

    squares = jnp.sum(mixed * mixed, axis=1, keepdims=True)
    send_sum[...] = jnp.sum(jnp.where(diagonal, squares, 0.0), axis=0, keepdims=True)
    sums = [
        remote(send_sum, recv_sum.at[o], s_sum.at[o], r_sum.at[o], {"tp": ahead_tp[o]})
        for o in range(1, tp)
    ]
    pending += sums

    fifth = []

    def forward(g):
        for o in far_tp:
            fifth.append(
                remote(
                    recv4.at[pl.ds(g * group_size, group_size)],
                    recv5.at[o, pl.ds(g * group_size, group_size)],
                    s5.at[o, g], r5.at[o, g], {"tp": ahead_tp[o]},
                )
            )

    def relay(first_group, last_group):
        for g in range(first_group, last_group):
            for o in range(max(1, g * group_size), (g + 1) * group_size):
                fourth[ep - 1 - o].wait_recv()
            forward(g)

    relay(0, groups // 2)
    for copy in sums:
        copy.wait_recv()
    total = send_sum[...]
    for o in range(1, tp):
        total = total + recv_sum[o]
    scales = column(lax.rsqrt(total / width + epsilon))
    send_scale[...] = jnp.sum(held * scales, axis=0, keepdims=True)
    scaled = [
        remote(send_scale, recv_scale.at[o], s_scale.at[o], r_scale.at[o], {"ep": ahead_ep[o]})
        for o in reversed(range(1, ep))
    ]
    pending += scaled
    relay(groups // 2, groups)
    pending += fifth
    for i in (15, 16, 17):
        loads[i].wait()

    gate = jnp.zeros((slots, w_gate.shape[1]), WIDE)
    upper = gate
    for o in range(tp):
        if o:
            for g in range(groups):
                fifth[g * (tp - 1) + tp - 1 - o].wait_recv()
        for e in range(ep):
            pack[e * capacity:(e + 1) * capacity, :] = (recv5[o, e] if o else recv4[e]).astype(WIDE)
        arrived = pack[...].astype(NARROW)
        depth = pl.ds(
            pl.multiple_of(ahead_tp[o] * col_width, 128), col_width
        )
        gate = gate + jnp.dot(arrived, w_gate[depth, :], preferred_element_type=WIDE)
        upper = upper + jnp.dot(arrived, w_up[depth, :], preferred_element_type=WIDE)
    for copy in scaled:
        copy.wait_recv()
    slot_of = lax.broadcasted_iota(jnp.int32, (1, slots), 1) // capacity
    slot_scale = jnp.where(slot_of == 0, send_scale[...], 0.0)
    for o in range(1, ep):
        slot_scale = jnp.where(slot_of == o, recv_scale[o], slot_scale)
    slot_scale = column(slot_scale)
    gate = gate * slot_scale
    upper = upper * slot_scale
    hidden = (silu(gate) * upper).astype(NARROW)

    def block(o):
        return jnp.dot(
            hidden, w_down[:, columns(o)], preferred_element_type=WIDE
        ).astype(NARROW)

    sixth = []
    for o in far_tp:
        send6[o] = block(o)
        sixth.append(remote(send6.at[o], recv6.at[o], s6.at[o], r6.at[o], {"tp": ahead_tp[o]}))
    pending += sixth
    expert_out = block(0).astype(WIDE)
    for copy in sixth:
        copy.wait_recv()
    for o in range(1, tp):
        expert_out = expert_out + recv6[o].astype(WIDE)
    pack_out[...] = expert_out.astype(NARROW).astype(WIDE)

    seventh = []
    for o in range(1, ep):
        send7[o] = pack_out[o * capacity:(o + 1) * capacity, :].astype(NARROW)
    for o in reversed(range(1, ep)):
        seventh.append(
            remote(send7.at[o], recv7.at[o], s7.at[o], r7.at[o], {"ep": behind_ep[o]})
        )
    pending += seventh
    for copy in seventh:
        copy.wait_recv()
    for o in range(1, ep):
        pack_out[o * capacity:(o + 1) * capacity, :] = recv7[o].astype(WIDE)
    moe_sum = jnp.dot(
        combine, pack_out[...], precision=lax.Precision.HIGHEST, preferred_element_type=WIDE
    )
    out_ref[...] = (mixed + moe_sum).astype(NARROW)
    for copy in pending:
        copy.wait_send()


def on_device(
    tokens, norm_gain, w_query, w_key, w_decay, w_value, w_outgate, decay_rate, state, head_gain,
    w_output, moe_gain, expert_ids, group_prob, inner_prob, w_gate, w_up, w_down,
):
    ep = lax.axis_size("ep")
    tp = lax.axis_size("tp")
    rows, width = tokens.shape
    top = expert_ids.shape[1]
    capacity = 2 * rows * top // ep
    slots = ep * capacity
    col_width = width // tp
    project_cols = 3 * w_query.shape[1] + 2 * w_value.shape[1]
    hidden = w_gate.shape[2]
    operands = (
        tokens, norm_gain.reshape(1, -1), w_query, w_key, w_decay, w_value, w_outgate,
        decay_rate.reshape(1, -1), state, head_gain.reshape(1, -1), w_output,
        moe_gain.reshape(1, -1), expert_ids.T, group_prob.reshape(1, -1), inner_prob.T, w_gate, w_up,
        w_down,
    )
    vmem = pltpu.VMEM
    local = [
        vmem((rows, width), NARROW),
        vmem((1, width), WIDE),
        vmem((w_query.shape[0], project_cols), NARROW),
        vmem((1, decay_rate.shape[0]), WIDE),
        vmem(state.shape, WIDE),
        vmem((1, head_gain.shape[0]), WIDE),
        vmem(w_output.shape, NARROW),
        vmem((1, width), WIDE),
        vmem((top, rows), jnp.int32),
        vmem((1, rows), WIDE),
        vmem((top, rows), WIDE),
        vmem((width, hidden), NARROW),
        vmem((width, hidden), NARROW),
        vmem((hidden, width), NARROW),
    ]
    buffers = [
        vmem((ep, rows, width // ep), NARROW),
        vmem((ep, rows, width // ep), NARROW),
        vmem((ep // 2, rows, project_cols), NARROW),
        vmem((ep // 2, rows, project_cols), NARROW),
        vmem((ep // 2, rows, project_cols), NARROW),
        vmem((ep // 2, rows, project_cols), NARROW),
        vmem((rows, state.shape[3]), WIDE),
        vmem((tp, rows, col_width), NARROW),
        vmem((tp, rows, col_width), NARROW),
        vmem((slots, col_width), WIDE),
        vmem((ep, capacity, col_width), NARROW),
        vmem((ep, capacity, col_width), NARROW),
        vmem((tp, ep, capacity, col_width), NARROW),
        vmem((1, rows), WIDE),
        vmem((tp, 1, rows), WIDE),
        vmem((1, slots), WIDE),
        vmem((ep, 1, slots), WIDE),
        vmem((tp, slots, col_width), NARROW),
        vmem((tp, slots, col_width), NARROW),
        vmem((slots, col_width), WIDE),
        vmem((ep, capacity, col_width), NARROW),
        vmem((ep, capacity, col_width), NARROW),
    ]
    dma = pltpu.SemaphoreType.DMA
    along_ep, along_tp = [dma((ep,))] * 2, [dma((tp,))] * 2
    semaphores = (
        [dma((len(operands),))] + along_ep + along_ep + along_tp + along_ep
        + [dma((tp, min(ep, 8)))] * 2 + along_tp + along_ep + along_tp + along_ep
    )
    return pl.pallas_call(
        functools.partial(layer, ep, tp, capacity),
        out_shape=pltpu.VMEM((rows, col_width), NARROW),
        in_specs=[pl.BlockSpec(memory_space=pl.ANY)] * len(operands),
        out_specs=pl.BlockSpec(memory_space=pltpu.VMEM),
        scratch_shapes=local + buffers + semaphores,
        compiler_params=pltpu.CompilerParams(
            collective_id=0, has_side_effects=True, vmem_limit_bytes=60 * 1024 * 1024
        ),
    )(*operands)


def solution(mesh):
    placed = (
        P("ep", None),
        P(),
        P("ep", "tp"),
        P("ep", "tp"),
        P("ep", "tp"),
        P("ep", "tp"),
        P("ep", "tp"),
        P("tp"),
        P("ep", "tp", None, None),
        P(),
        P("tp", None),
        P(),
        P("ep", None),
        P("ep"),
        P("ep", None),
        P("ep", None, "tp"),
        P("ep", None, "tp"),
        P("ep", "tp", None),
    )
    return jax.shard_map(
        on_device, mesh=mesh, in_specs=placed, out_specs=P("ep", "tp"), check_vma=False
    )
```
